512 devices in a mesh: grp: 2 (over y), sp: 64 (over z, core), tp: 4 (over x).
Axes of the slice: x: 4, y: 2, z: 32, core: 2. Of those that a mesh axis runs over, the one named last changes fastest.
The devices are a block of a 4x8x32 slice.
Arguments:
- tokens: bfloat16 [49152, 2048], P(('grp', 'sp')), parts along dimension 0, may hold values from -6 to 6
- norm_gain: float32 [2, 2048], replicated, may hold values from 0.1 to 1.9
- entry_weight: bfloat16 [2, 2048, 2048], P(None, 'sp', 'tp'), may hold values from -0.125 to 0.125
- mix_weight: bfloat16 [2, 4, 512, 512], P(None, 'tp'), may hold values from -0.25 to 0.25
- pool_gain: float32 [2, 2048], P(None, 'tp'), may hold values from 0.1 to 1.9
- back_weight: bfloat16 [2, 2048, 2048], P(None, 'tp', 'sp'), may hold values from -0.25 to 0.25
Outputs:
- result_tokens: bfloat16 [49152, 2048], P(('grp', 'sp')), parts along dimension 0
The draws below stay inside these ranges and needn't reach their ends.
There are 2 independent parts, one for each index of `grp`. The reference program is written for one: setup_inputs(seed, part) draws one part's arguments, and reference() takes and returns one part's arrays. A program takes and returns all parts, laid end to end along the dimension named above; an argument that names none is the same for every part. Nothing has to cross between parts.
All inputs are finite; a program needn't handle non-finite values.
Results may differ from the reference program's by a relative error of at most 0.018.
Values may be sent and summed in bfloat16 or wider, within the bound.
A program may use at most 64 MiB of HBM per device.

```python
import jax
import jax.numpy as jnp
from jax import lax

D = 2048
GROUPS = 4
POOL_W = 2048
GROUP_W = 512
LAYERS = 2
LENGTH = 24576
N_TP = 4


def steps_of(own_key, extent, shards, low, largest):
    factor_of = 1.0
    for axis_at, parts in shards:
        heights = jax.random.uniform(jax.random.fold_in(jax.random.fold_in(own_key, 6), axis_at), (parts,), jnp.float32, low / len(shards), largest / len(shards))
        factor_of = factor_of * jnp.repeat(jnp.exp(heights), extent[axis_at] // parts).reshape((-1,) + (1,) * (len(extent) - 1 - axis_at))
    return factor_of


def normal_values(stream_key, dims, width, bound, split=(), held_as=jnp.bfloat16):
    values = jax.random.normal(stream_key, dims, jnp.float32) * width
    if len(split) > 0:
        values = steps_of(stream_key, dims, split, -0.22, 0.18) * values
    return jnp.clip(values, min=-bound, max=bound).astype(held_as)


def setup_inputs(seed: int = 0, part: int = 0) -> dict:
    splits = jax.random.split(jax.random.key(seed), 7)
    part_splits = jax.random.split(jax.random.fold_in(splits[6], part), 7)
    return {
        "tokens": normal_values(part_splits[0], (LENGTH, D), 1.0, 6.0, ((0, 64),)),
        "norm_gain": jnp.clip(1.0 + 0.18 * jax.random.normal(splits[1], (LAYERS, D), jnp.float32), 0.1, 1.9),
        "entry_weight": normal_values(splits[2], (LAYERS, D, POOL_W), D ** -0.5, 0.125, ((1, 64), (2, 4))),
        "mix_weight": normal_values(splits[3], (LAYERS, GROUPS, GROUP_W, GROUP_W), GROUP_W ** -0.5, 0.25, ((1, 4),)),
        "pool_gain": jnp.clip(1.0 + 0.18 * jax.random.normal(splits[4], (LAYERS, POOL_W), jnp.float32), 0.1, 1.9),
        "back_weight": normal_values(splits[5], (LAYERS, POOL_W, D), (POOL_W // 4) ** -0.5, 0.25, ((1, 4), (2, 64))),
    }


EPSILON = 1e-05

def window_mean(padded, positions, halves, total_length, reach):
    row_count = positions.shape[0]
    summed = jnp.zeros((row_count,) + padded.shape[1:], jnp.float32)
    for offset in range(-reach, reach):
        inside = ((offset >= -halves) & (offset < halves)).astype(jnp.float32)
        summed = summed + padded[reach + offset:reach + offset + row_count] * inside[None, :, None]
    lower = jnp.maximum(positions[:, None] - halves[None, :], 0)
    upper = jnp.minimum(positions[:, None] + halves[None, :], total_length)
    counted = (upper - lower).astype(jnp.float32)
    return summed / counted[:, :, None]

def reference(tokens, norm_gain, entry_weight, mix_weight, pool_gain, back_weight):
    reach = 2 ** (GROUPS - 1)
    halves = jnp.left_shift(jnp.int32(1), jnp.arange(GROUPS, dtype=jnp.int32))
    positions = jnp.arange(LENGTH, dtype=jnp.int32)
    block_width = POOL_W // N_TP
    state = tokens
    for layer in range(LAYERS):
        values = state.astype(jnp.float32)
        scaled = values * lax.rsqrt(lax.optimization_barrier(jnp.mean(values * values, axis=-1, keepdims=True)) + EPSILON)
        normed = (scaled * norm_gain[layer].astype(jnp.float32)).astype(jnp.bfloat16)
        pooled_in = jnp.dot(normed, entry_weight[layer], preferred_element_type=jnp.float32).astype(jnp.bfloat16)
        grouped = pooled_in.reshape(LENGTH, GROUPS, GROUP_W).astype(jnp.float32)
        padded = jnp.pad(grouped, ((reach, reach), (0, 0), (0, 0)))
        means = window_mean(padded, positions, halves, LENGTH, reach)
        differ = (means - grouped).astype(jnp.bfloat16)
        mixed = jnp.einsum('tgc,gcd->tgd', differ.astype(jnp.float32), mix_weight[layer].astype(jnp.float32))
        mixed = (mixed.reshape(LENGTH, POOL_W) * pool_gain[layer].astype(jnp.float32)).astype(jnp.bfloat16)
        total = values
        for block in range(N_TP):
            term = jnp.dot(mixed[:, block * block_width:(block + 1) * block_width], back_weight[layer, block * block_width:(block + 1) * block_width], preferred_element_type=jnp.float32)
            total = total + lax.optimization_barrier(term.astype(jnp.bfloat16)).astype(jnp.float32)
        state = total.astype(jnp.bfloat16)
    return state
```

```python
import functools

import jax
import jax.numpy as jnp
from jax import lax
from jax.experimental import pallas as pl
from jax.experimental.pallas import tpu as pltpu
from jax.sharding import PartitionSpec as P

GROUPS = 4
LAYERS = 2
EPSILON = 1e-05
MESH = pl.DeviceIdType.MESH
REACH = 2 ** (GROUPS - 1)
HALO = LAYERS * REACH
CHUNKS = 2
CORES = 2
PIECES = 2 * LAYERS
TILE = 16


def half_rows(rows):
    return (rows // 2 + TILE - 1) // TILE * TILE


def kernel(
    nsp, ntp, tok, weights, norm_gain, mix, pool_gain, out,
    ext, w_all, normed, pooled, mixed,
    term0, term1, acc0, acc1, via_left0, via_left1, via_right0, via_right1,
    from_left0, from_left1, from_right0, from_right1, state0, state1,
    z_send, z_recv, p_send, p_recv, h_send, h_recv, x_send, x_recv, l_sem, o_sem,
):
    rows, model = tok.shape
    width = model // ntp // CHUNKS
    block = weights.shape[1]
    nz = nsp // CORES
    sp = lax.axis_index("sp")
    me = lax.axis_index("tp")
    z, core = sp // CORES, lax.rem(sp, CORES)
    total_length = nsp * rows
    term, acc = (term0, term1), (acc0, acc1)
    via_left, via_right = (via_left0, via_left1), (via_right0, via_right1)
    from_left, from_right = (from_left0, from_left1), (from_right0, from_right1)
    state = (state0, state1)

    def around(value, size):
        return lax.rem(value + size, size)

    z_next = (around(z + 1, nz) * CORES + core, around(z - 1, nz) * CORES + core)
    partner = z * CORES + (1 - core)
    seq_left, seq_right = around(sp - 1, nsp), around(sp + 1, nsp)
    tp_right, tp_left, tp_far = around(me + 1, ntp), around(me - 1, ntp), around(me + 2, ntp)

    barrier = pltpu.get_barrier_semaphore()
    far = jnp.where(core == 0, seq_left, seq_right)
    for target in (z_next[0], z_next[1], partner, far):
        pl.semaphore_signal(barrier, inc=1, device_id={"sp": target}, device_id_type=MESH)
    for target in (tp_right, tp_left):
        pl.semaphore_signal(barrier, inc=1, device_id={"tp": target}, device_id_type=MESH)

    def block_rows(slot):
        return pl.ds(pl.multiple_of(slot * block, block), block)

    own = pltpu.make_async_copy(weights, w_all.at[:, block_rows(sp), :], l_sem.at[0])
    own.start()
    own_tokens = pltpu.make_async_copy(tok, ext.at[pl.ds(HALO, rows)], l_sem.at[1])
    own_tokens.start()
    own.wait()
    pl.semaphore_wait(barrier, 6)

    def z_copy(d, step, p, distance):
        origin = around(z - distance, nz) if d == 0 else lax.rem(z + distance, nz)
        where = w_all.at[p, block_rows(origin * CORES + core), :]
        return pltpu.make_async_remote_copy(
            src_ref=where, dst_ref=where, send_sem=z_send.at[d, step, p], recv_sem=z_recv.at[d, step, p],
            device_id={"sp": z_next[d]}, device_id_type=MESH,
        )

    def p_copy(j, p, of_core):
        where = w_all.at[p, block_rows(lax.rem(z + j, nz) * CORES + of_core), :]
        return pltpu.make_async_remote_copy(
            src_ref=where, dst_ref=where, send_sem=p_send.at[j, p], recv_sem=p_recv.at[j, p],
            device_id={"sp": partner}, device_id_type=MESH,
        )

    steps = (nz // 2, nz - 1 - nz // 2)

    def landed(d, step, p):
        z_copy(d, step, p, step + 1).wait_recv()

    def share(d, step, p):
        p_copy(nz - 1 - step if d == 0 else step + 1, p, core).start()

    for p in range(PIECES):
        for d in range(2):
            z_copy(d, 0, p, 0).start()
    h_left = pltpu.make_async_remote_copy(
        src_ref=tok.at[pl.ds(0, HALO)], dst_ref=ext.at[pl.ds(HALO + rows, HALO)],
        send_sem=h_send.at[0], recv_sem=h_recv.at[0], device_id={"sp": seq_left}, device_id_type=MESH,
    )
    h_right = pltpu.make_async_remote_copy(
        src_ref=tok.at[pl.ds(rows - HALO, HALO)], dst_ref=ext.at[pl.ds(0, HALO)],
        send_sem=h_send.at[1], recv_sem=h_recv.at[1], device_id={"sp": seq_right}, device_id_type=MESH,
    )
    h_left.start()
    h_right.start()
    for p in range(PIECES):
        p_copy(0, p, core).start()

    own_tokens.wait()
    h_left.wait_recv()
    h_right.wait_recv()

    @pl.loop(0, ext.shape[0] // TILE)
    def _(t):
        where = pl.ds(pl.multiple_of(t * TILE, TILE), TILE)
        values = ext[where, :].astype(jnp.float32)
        scale = lax.rsqrt(jnp.mean(values * values, axis=-1, keepdims=True) + EPSILON)
        normed[where, :] = (values * scale * norm_gain[0:1, :]).astype(jnp.bfloat16)

    @pl.loop(1, steps[1])
    def _(step):
        for p in range(PIECES):
            for d in range(2):
                landed(d, step - 1, p)
                z_copy(d, step, p, step).start()
                share(d, step - 1, p)

    last = steps[1]
    for p in range(PIECES):
        landed(0, last - 1, p)
        z_copy(0, last, p, last).start()
        share(0, last - 1, p)
        landed(1, last - 1, p)
        share(1, last - 1, p)
    for p in range(PIECES):
        landed(0, last, p)
        share(0, last, p)

    @pl.loop(0, nz)
    def _(j):
        for p in range(PIECES):
            p_copy(j, p, 1 - core).wait_recv()

    half_window = jnp.left_shift(jnp.int32(1), me)

    for layer in range(LAYERS):
        extent = rows + 2 * HALO - 2 * REACH * layer
        count = extent - 2 * REACH
        half = half_rows(count)
        offset = HALO - REACH * layer
        first, second = pl.ds(0, half), pl.ds(half, count - half)

        if layer > 0:
            before = state[layer - 1]

            @pl.loop(0, extent // TILE)
            def _(t, before=before, layer=layer):
                where = pl.ds(pl.multiple_of(t * TILE, TILE), TILE)
                parts = [
                    before[k, c, where, :].astype(jnp.float32) for k in range(ntp) for c in range(CHUNKS)
                ]
                squares = parts[0] * parts[0]
                for part in parts[1:]:
                    squares = squares + part * part
                mean = jnp.sum(squares, axis=-1, keepdims=True) / model
                scale = lax.rsqrt(mean + EPSILON)
                for n, part in enumerate(parts):
                    columns = pl.ds(n * width, width)
                    gain = norm_gain[layer : layer + 1, columns]
                    normed[where, columns] = (part * scale * gain).astype(jnp.bfloat16)

        entered = jnp.dot(normed[0:extent, :], w_all[2 * layer], preferred_element_type=jnp.float32)
        at = sp * rows - offset + lax.broadcasted_iota(jnp.int32, (extent, 1), 0)
        inside = (at >= 0) & (at < total_length)
        pooled[0:extent, :] = jnp.where(inside, entered, 0.0).astype(jnp.bfloat16)

        here = lax.broadcasted_iota(jnp.int32, (count, extent), 0) + REACH
        there = lax.broadcasted_iota(jnp.int32, (count, extent), 1)
        apart = there - here
        band = jnp.where((apart >= -half_window) & (apart < half_window), 1.0, 0.0).astype(jnp.bfloat16)
        values = pooled[0:extent, :]
        summed = jnp.dot(band, values, preferred_element_type=jnp.float32)
        at = sp * rows - offset + REACH + lax.broadcasted_iota(jnp.int32, (count, 1), 0)
        lower = jnp.maximum(at - half_window, 0)
        upper = jnp.minimum(at + half_window, total_length)
        counted = jnp.maximum(upper - lower, 1).astype(jnp.float32)
        differ = summed / counted - values.astype(jnp.float32)[REACH : REACH + count]
        product = jnp.dot(differ.astype(jnp.bfloat16), mix[layer], preferred_element_type=jnp.float32)
        mixed[0:count, :] = (product * pool_gain[layer : layer + 1, :]).astype(jnp.bfloat16)

        def x_copy(c, m, layer=layer, first=first, second=second):
            t, a, s = term[layer], acc[layer], state[layer]
            source, target, to = (
                (t.at[c, tp_far, first], via_left[layer].at[c], tp_right),
                (t.at[c, tp_far, second], via_right[layer].at[c], tp_left),
                (t.at[c, tp_right, second], from_left[layer].at[c, second], tp_right),
                (t.at[c, tp_left, first], from_right[layer].at[c, first], tp_left),
                (a.at[c, first], from_left[layer].at[c, first], tp_right),
                (a.at[c, second], from_right[layer].at[c, second], tp_left),
                (s.at[me, c], s.at[me, c], tp_right),
                (s.at[me, c], s.at[me, c], tp_left),
                (s.at[tp_left, c, first], s.at[tp_left, c, first], tp_right),
                (s.at[tp_right, c, second], s.at[tp_right, c, second], tp_left),
            )[m]
            return pltpu.make_async_remote_copy(
                src_ref=source, dst_ref=target, send_sem=x_send.at[layer, c, m], recv_sem=x_recv.at[layer, c, m],
                device_id={"tp": to}, device_id_type=MESH,
            )

        def x_landed(c, m, layer=layer, first=first, second=second):
            s = state[layer]
            target = (
                via_left[layer].at[c],
                via_right[layer].at[c],
                from_left[layer].at[c, second],
                from_right[layer].at[c, first],
                from_left[layer].at[c, first],
                from_right[layer].at[c, second],
                s.at[tp_left, c],
                s.at[tp_right, c],
                s.at[tp_far, c, first],
                s.at[tp_far, c, second],
            )[m]
            pltpu.make_async_remote_copy(
                src_ref=target, dst_ref=target, send_sem=x_send.at[layer, c, m], recv_sem=x_recv.at[layer, c, m],
                device_id={"tp": tp_right}, device_id_type=MESH,
            ).wait_recv()

        def columns_of(k, c):
            return pl.ds(pl.multiple_of((k * CHUNKS + c) * width, width), width)

        def put(k, c, layer=layer):
            if layer == LAYERS - 1:
                pltpu.make_async_copy(state[layer].at[k, c], out.at[:, columns_of(k, c)], o_sem.at[k, c]).start()

        def compute_term(c, k, layer=layer, count=count):
            value = lax.dot_general(
                mixed[0:count, :], w_all[2 * layer + 1, columns_of(k, c), :], (((1,), (1,)), ((), ())),
                preferred_element_type=jnp.float32,
            )
            term[layer][c, k] = value.astype(jnp.bfloat16)

        for c in range(CHUNKS):
            compute_term(c, tp_far)
            x_copy(c, 0).start()
            x_copy(c, 1).start()
            compute_term(c, tp_right)
            x_copy(c, 2).start()
            compute_term(c, tp_left)
            x_copy(c, 3).start()
            compute_term(c, me)
        for c in range(CHUNKS):
            x_landed(c, 0)
            joined = term[layer][c, tp_right, first].astype(jnp.float32) + via_left[layer][c].astype(jnp.float32)
            acc[layer][c, first] = joined.astype(jnp.bfloat16)
            x_copy(c, 4).start()
            x_landed(c, 1)
            joined = term[layer][c, tp_left, second].astype(jnp.float32) + via_right[layer][c].astype(jnp.float32)
            acc[layer][c, second] = joined.astype(jnp.bfloat16)
            x_copy(c, 5).start()
        for c in range(CHUNKS):
            for m in (2, 3, 4, 5):
                x_landed(c, m)
            if layer == 0:
                kept = ext[:, columns_of(me, c)].astype(jnp.float32)
            else:
                kept = state[layer - 1][me, c].astype(jnp.float32)
            total = kept[REACH : REACH + count] + term[layer][c, me].astype(jnp.float32)
            total = total + from_left[layer][c].astype(jnp.float32) + from_right[layer][c].astype(jnp.float32)
            state[layer][me, c] = total.astype(jnp.bfloat16)
            x_copy(c, 6).start()
            x_copy(c, 7).start()
            put(me, c)
        for c in range(CHUNKS):
            x_landed(c, 6)
            x_copy(c, 8).start()
            put(tp_left, c)
            x_landed(c, 7)
            x_copy(c, 9).start()
            put(tp_right, c)
        for c in range(CHUNKS):
            x_landed(c, 8)
            x_landed(c, 9)
            put(tp_far, c)
        for c in range(CHUNKS):
            for m in range(10):
                x_copy(c, m).wait_send()

    h_left.wait_send()
    h_right.wait_send()

    @pl.loop(0, steps[1])
    def _(step):
        for p in range(PIECES):
            for d in range(2):
                z_copy(d, step, p, step).wait_send()

    @pl.loop(0, nz)
    def _(j):
        for p in range(PIECES):
            p_copy(j, p, core).wait_send()

    for p in range(PIECES):
        z_copy(0, last, p, last).wait_send()
    for k in range(ntp):
        for c in range(CHUNKS):
            pltpu.make_async_copy(state[-1].at[k, c], out.at[:, columns_of(k, c)], o_sem.at[k, c]).wait()


def per_device(nsp, ntp, tokens, norm_gain, entry_weight, mix_weight, pool_gain, back_weight):
    rows, model = tokens.shape
    pool = entry_weight.shape[2]
    turned = jnp.swapaxes(back_weight, 1, 2)
    weights = jnp.stack([entry_weight, turned], axis=1).reshape(PIECES, entry_weight.shape[1], pool)
    nz = nsp // CORES
    width = model // ntp // CHUNKS
    extent = rows + 2 * HALO
    counts = [rows + 2 * HALO - 2 * REACH * (layer + 1) for layer in range(LAYERS)]

    def per_layer(shape_of):
        return [pltpu.VMEM(shape_of(count), jnp.bfloat16) for count in counts]

    scratch = [
        pltpu.VMEM((extent, model), jnp.bfloat16),
        pltpu.VMEM((PIECES, model, pool), jnp.bfloat16),
        pltpu.VMEM((extent, model), jnp.bfloat16),
        pltpu.VMEM((extent, pool), jnp.bfloat16),
        pltpu.VMEM((extent, pool), jnp.bfloat16),
        *per_layer(lambda count: (CHUNKS, ntp, count, width)),
        *per_layer(lambda count: (CHUNKS, count, width)),
        *per_layer(lambda count: (CHUNKS, half_rows(count), width)),
        *per_layer(lambda count: (CHUNKS, count - half_rows(count), width)),
        *per_layer(lambda count: (CHUNKS, count, width)),
        *per_layer(lambda count: (CHUNKS, count, width)),
        *per_layer(lambda count: (ntp, CHUNKS, count, width)),
        pltpu.SemaphoreType.DMA((2, nz // 2, PIECES)),
        pltpu.SemaphoreType.DMA((2, nz // 2, PIECES)),
        pltpu.SemaphoreType.DMA((nz, PIECES)),
        pltpu.SemaphoreType.DMA((nz, PIECES)),
        pltpu.SemaphoreType.DMA((2,)),
        pltpu.SemaphoreType.DMA((2,)),
        pltpu.SemaphoreType.DMA((LAYERS, CHUNKS, 10)),
        pltpu.SemaphoreType.DMA((LAYERS, CHUNKS, 10)),
        pltpu.SemaphoreType.DMA((2,)),
        pltpu.SemaphoreType.DMA((ntp, CHUNKS)),
    ]
    anywhere = pl.BlockSpec(memory_space=pl.ANY)
    vmem = pl.BlockSpec(memory_space=pltpu.VMEM)
    return pl.pallas_call(
        functools.partial(kernel, nsp, ntp),
        out_shape=jax.ShapeDtypeStruct((rows, model), jnp.bfloat16),
        in_specs=[anywhere, anywhere, vmem, vmem, vmem],
        out_specs=anywhere,
        scratch_shapes=scratch,
        compiler_params=pltpu.CompilerParams(
            collective_id=0, has_side_effects=True, vmem_limit_bytes=56 * 2**20
        ),
        name="mixer",
    )(tokens, weights, norm_gain, mix_weight[:, 0], pool_gain)


def solution(mesh):
    body = functools.partial(per_device, mesh.shape["sp"], mesh.shape["tp"])
    return jax.shard_map(
        body,
        mesh=mesh,
        in_specs=(
            P(("grp", "sp"), None),
            P(),
            P(None, "sp", "tp"),
            P(None, "tp", None, None),
            P(None, "tp"),
            P(None, "tp", "sp"),
        ),
        out_specs=P(("grp", "sp"), None),
        check_vma=False,
    )
```
